32 devices in a mesh: sp: 8 (over z, core), tp: 4 (over y, x).
Axes of the slice: x: 2, y: 2, z: 4, core: 2. Of those that a mesh axis runs over, the one named last changes fastest.
Arguments:
- query_rows: bfloat16 [2048, 2048], P('sp', 'tp'), may hold values from -1000 to 1000
- key_rows: bfloat16 [2048, 256], P('sp'), may hold values from -6 to 6
- value_rows: bfloat16 [2048, 256], P('sp'), may hold values from -6 to 6
- sink_logits: float32 [32], P('tp'), may hold values from 1 to 6
- out_weight: bfloat16 [2048, 2048], P('tp'), may hold values from -0.375 to 0.375
- stream_in: bfloat16 [2048, 2048], P('sp'), may hold values from -6 to 6
- norm_gain: float32 [2048], replicated, may hold values from 0.1 to 1.9
- routes: int32 [2048, 2], P('sp'), may hold values from 0 to 7, all different within a row; in each aligned block of 256 rows (0 to 255, 256 to 511, ...) at most 96 rows name the same one
- route_weights: float32 [2048, 2], P('sp'), may hold values from 0.2 to 1
- gate_weight: bfloat16 [8, 2048, 4096], P('sp', None, 'tp'), may hold values from -0.125 to 0.125
- up_weight: bfloat16 [8, 2048, 4096], P('sp', None, 'tp'), may hold values from -0.125 to 0.125
- down_weight: bfloat16 [8, 4096, 2048], P('sp', 'tp'), may hold values from -0.09375 to 0.09375
Outputs:
- layer_out: bfloat16 [2048, 2048], P(('sp', 'tp'))
The draws below stay inside these ranges and needn't reach their ends.
Inputs may be any that keep to these rules, and one draw needn't show every extreme that they name: `routes`: each row names 2 different experts. Within the rows of one device (256 aligned rows) no expert is named more than 96 times, a bound that some block reaches.
All inputs are finite; a program needn't handle non-finite values.
Results may differ from the reference program's by a relative error of at most 0.015.
Values may be sent and summed in bfloat16 or wider, within the bound.
A program may use at most 64 MiB of HBM per device.

```python
import math
import jax
import jax.numpy as jnp
import numpy as np
from jax import lax

D = 2048
HEAD_DIM = 64
HEADS = 32
KV_HEADS = 4
REP = 8
WINDOW = 128
EXPERT_FF = 4096
TOPK = 2
TOK_SP = 256
TOKENS = 2048
EXPERTS = 8
CAP = 96
N_SP = 8
N_TP = 4


def drawn_pair(key):
    key_draw = jnp.clip(jax.random.normal(jax.random.fold_in(key, 11), (TOKENS, KV_HEADS, HEAD_DIM), jnp.float32), -6.0, 6.0)
    queries = jnp.clip(jax.random.normal(jax.random.fold_in(key, 12), (TOKENS, KV_HEADS, REP, HEAD_DIM), jnp.float32), -6.0, 6.0)
    return (key_draw, queries)


def draw_query_rows(key, part):
    key_draw, queries = drawn_pair(key)
    return queries.reshape(TOKENS, HEADS * HEAD_DIM).astype(jnp.bfloat16)


def draw_key_rows(key, part):
    key_draw, queries = drawn_pair(key)
    return key_draw.reshape(TOKENS, KV_HEADS * HEAD_DIM).astype(jnp.bfloat16)


def block_levels(rng, shape, cuts, smallest, top_value):
    level = 1.0
    for axis_at, parts in cuts:
        heights = jax.random.uniform(jax.random.fold_in(jax.random.fold_in(rng, 6), axis_at), (parts,), jnp.float32, smallest / len(cuts), top_value / len(cuts))
        level = level * jnp.repeat(jnp.exp(heights), shape[axis_at] // parts).reshape((-1,) + (1,) * (len(shape) - 1 - axis_at))
    return level


def assign_block(stream_key, own, number, rows, amount, top, limit, skew):
    order = jax.random.permutation(stream_key, amount)
    heavy_load, common = load_shares(amount, rows * top, limit, skew, True), load_shares(amount, rows * top, limit, skew, False)
    places = jnp.arange(amount)

    def named(sizes, rotation):
        used = int((sizes > 0).sum())
        fixed = max(1, used // 4)
        shifted = fixed + (places - fixed + rotation * (used - fixed)) % max(1, amount - fixed)
        return jnp.zeros((amount,), jnp.int32).at[order[jnp.where(places < fixed, places, shifted)]].set(jnp.asarray(sizes, jnp.int32))

    sizes = jnp.where(number % 4 == 0, named(heavy_load, number // 4), named(common, number - number // 4 - 1))
    mixed = jax.random.permutation(jax.random.fold_in(own, 3), amount)
    giver, sink = mixed[0:amount // 2 * 2:2], mixed[1:amount // 2 * 2:2]
    room = jnp.minimum(sizes[giver] - 1, limit - sizes[sink]) // 2
    room = jnp.where((giver == order[0]) | (sink == order[0]) | (sizes[sink] == 0), 0, jnp.maximum(room, 0))
    shifted = jax.random.randint(jax.random.fold_in(own, 4), (amount // 2,), 0, 1 << 20) % (room + 1)
    sizes = sizes.at[giver].add(-shifted).at[sink].add(shifted)
    members = jnp.searchsorted(jnp.cumsum(sizes), jnp.arange(rows * top), side="right").astype(jnp.int32)
    listing = members.reshape(top, rows).T
    listing = listing[jax.random.permutation(jax.random.fold_in(own, 1), rows)]
    rotation = jax.random.randint(jax.random.fold_in(own, 2), (rows, 1), 0, top)
    return jnp.take_along_axis(listing, (jnp.arange(top)[None, :] + rotation) % top, axis=1)


def load_shares(count, total, bound, skew, full):
    portions = [(1 << 20) // math.isqrt(grade ** skew) + 1 for grade in range(1, count + 1)]
    largest = bound if full else min(bound, max(-(-total // count), total * portions[0] // sum(portions)))
    least = 1 if total - largest >= count - 1 else 0
    given, rest = [largest] + [least] * (count - 1), total - largest - least * (count - 1)
    while rest > 0:
        candidates = [i for i in range(1, count) if given[i] < largest] or [i for i in range(1, count) if given[i] < bound]
        whole, budget = sum([portions[i] for i in candidates]), rest
        for i in candidates:
            extra = min(bound - given[i], max(1, budget * portions[i] // whole), rest)
            given[i] = given[i] + extra
            rest = rest - extra
    return np.array(given)


def scatter_about(own_key, shape, scale, bound, pieces=(), held_as=jnp.bfloat16):
    factor_of = block_levels(own_key, shape, pieces, -0.22, 0.18) if pieces else 1.0
    result = jax.random.normal(own_key, shape, jnp.float32) * scale * factor_of
    return jnp.minimum(jnp.maximum(result, -bound), bound).astype(held_as)


def setup_inputs(seed: int = 0) -> dict:
    keys = jax.random.split(jax.random.key(seed), 13)
    query_rows = draw_query_rows(jax.random.fold_in(keys[12], 71), 0)
    key_rows = draw_key_rows(jax.random.fold_in(keys[12], 71), 0)
    value_rows = scatter_about(keys[2], (TOKENS, KV_HEADS * HEAD_DIM), 1.0, 6.0, ((0, 8),))
    sink_logits = jnp.clip(1.0 + 5.0 * jax.random.uniform(keys[3], (HEADS,), jnp.float32) ** block_levels(keys[3], (HEADS,), ((0, 4),), -0.2, 0.2), 1.0, 6.0)
    out_weight = scatter_about(keys[4], (HEADS * HEAD_DIM, D), (HEADS * HEAD_DIM // 8) ** -0.5, 0.375, ((0, 4),))
    stream_in = scatter_about(keys[5], (TOKENS, D), 1.0, 6.0, ((0, 8),))
    norm_gain = jnp.clip(1.0 + 0.18 * jax.random.normal(keys[6], (D,), jnp.float32), 0.1, 1.9)
    routes_keys = jax.random.split(jax.random.fold_in(keys[7], 1), TOKENS // TOK_SP)
    routes_turns = jax.random.permutation(jax.random.fold_in(keys[7], 3), TOKENS // TOK_SP)
    routes = jax.vmap(lambda own, number: assign_block(jax.random.fold_in(keys[7], 2), own, number, TOK_SP, EXPERTS, TOPK, CAP, 1))(routes_keys, routes_turns).reshape((TOKENS, TOPK))
    route_weights = jnp.clip(0.2 + 0.8 * jax.random.uniform(keys[8], (TOKENS, TOPK), jnp.float32) ** block_levels(keys[8], (TOKENS, TOPK), ((0, 8),), -0.2, 0.2), 0.2, 1.0)
    gate_weight = scatter_about(keys[9], (EXPERTS, D, EXPERT_FF), D ** -0.5, 0.125, ((0, 8), (2, 4)))
    up_weight = scatter_about(keys[10], (EXPERTS, D, EXPERT_FF), D ** -0.5, 0.125, ((0, 8), (2, 4)))
    down_weight = scatter_about(keys[11], (EXPERTS, EXPERT_FF, D), EXPERT_FF ** -0.5, 0.09375, ((0, 8), (1, 4)))
    return dict(query_rows=query_rows, key_rows=key_rows, value_rows=value_rows, sink_logits=sink_logits, out_weight=out_weight, stream_in=stream_in, norm_gain=norm_gain, routes=routes, route_weights=route_weights, gate_weight=gate_weight, up_weight=up_weight, down_weight=down_weight)


norm_eps = 1e-06

def route_targets(block_routes):
    flat_ids = block_routes.reshape(-1)
    onehot = (flat_ids[:, None] == jnp.arange(EXPERTS, dtype=jnp.int32)[None, :]).astype(jnp.int32)
    before = jnp.cumsum(onehot, axis=0) - onehot
    return (flat_ids * CAP + lax.optimization_barrier(jnp.sum(before * onehot, axis=1))).astype(jnp.int32)

def slot_table(block_targets):
    pair_token = (jnp.arange(block_targets.shape[0], dtype=jnp.int32) // TOPK).astype(jnp.int32)
    slot_token = jnp.zeros((EXPERTS * CAP,), jnp.int32).at[block_targets].set(pair_token)
    slot_live = jnp.zeros((EXPERTS * CAP,), jnp.int32).at[block_targets].set(1)
    return (slot_token, slot_live)

def attention(query_rows, key_rows, value_rows, sink_logits):
    tok_total = query_rows.shape[0]
    queries = query_rows.reshape(tok_total, KV_HEADS, REP, HEAD_DIM)
    key_heads = jnp.pad(key_rows.reshape(tok_total, KV_HEADS, HEAD_DIM), ((WINDOW, 0), (0, 0), (0, 0)))
    value_heads = jnp.pad(value_rows.reshape(tok_total, KV_HEADS, HEAD_DIM), ((WINDOW, 0), (0, 0), (0, 0)))
    block_rows = TOK_SP
    sink_col = sink_logits.astype(jnp.float32).reshape(KV_HEADS, REP, 1, 1)

    def one_block(first_row):
        query_block = lax.dynamic_slice_in_dim(queries, first_row, block_rows, 0).astype(jnp.float32)
        key_block = lax.dynamic_slice_in_dim(key_heads, first_row, block_rows + WINDOW, 0).astype(jnp.float32)
        value_block = lax.dynamic_slice_in_dim(value_heads, first_row, block_rows + WINDOW, 0).astype(jnp.float32)
        query_pos = first_row + jnp.arange(block_rows, dtype=jnp.int32)
        key_pos = first_row - WINDOW + jnp.arange(block_rows + WINDOW, dtype=jnp.int32)
        distance = query_pos[:, None] - key_pos[None, :]
        allowed = (distance >= 0) & (distance < WINDOW) & (key_pos >= 0)[None, :]
        scores = jnp.einsum('qgrd,kgd->grqk', query_block, key_block) * HEAD_DIM ** (-0.5)
        scores = jnp.where(allowed[None, None], scores, -1e+30)
        row_peak = jnp.maximum(lax.optimization_barrier(jnp.max(scores, axis=-1, keepdims=True)), sink_col)
        exp_terms = jnp.exp(scores - row_peak)
        denom_sum = lax.optimization_barrier(jnp.sum(exp_terms, axis=-1, keepdims=True)) + jnp.exp(sink_col - row_peak)
        attn_probs = (exp_terms / denom_sum).astype(jnp.bfloat16)
        attended = jnp.einsum('grqk,kgd->qgrd', attn_probs.astype(jnp.float32), value_block)
        return attended.astype(jnp.bfloat16).reshape(block_rows, HEADS * HEAD_DIM)
    starts = jnp.arange(tok_total // block_rows, dtype=jnp.int32) * block_rows
    return lax.map(one_block, starts).reshape(tok_total, HEADS * HEAD_DIM)

def reference(query_rows, key_rows, value_rows, sink_logits, out_weight, stream_in, norm_gain, routes, route_weights, gate_weight, up_weight, down_weight):
    attended = attention(query_rows, key_rows, value_rows, sink_logits)
    head_cols = HEADS * HEAD_DIM // N_TP

    def add_group(group_index, running):
        first_col = (jnp.asarray(group_index) * head_cols).astype(jnp.int32)
        piece = lax.dynamic_slice_in_dim(attended, first_col, head_cols, 1)
        weight_piece = lax.dynamic_slice_in_dim(out_weight, first_col, head_cols, 0)
        partial_value = jnp.dot(piece, weight_piece, preferred_element_type=jnp.float32).astype(jnp.bfloat16)
        return running + lax.optimization_barrier(partial_value).astype(jnp.float32)
    projected = lax.fori_loop(0, N_TP, add_group, jnp.zeros((TOKENS, D), jnp.float32))
    stream = (stream_in.astype(jnp.float32) + projected).astype(jnp.bfloat16)
    values = stream.astype(jnp.float32)
    normed = (values * lax.rsqrt(lax.optimization_barrier(jnp.mean(values * values, axis=-1, keepdims=True)) + norm_eps) * norm_gain.astype(jnp.float32)).astype(jnp.bfloat16)
    targets = jax.vmap(route_targets)(routes.reshape(N_SP, TOK_SP, TOPK))
    slot_token, slot_live = jax.vmap(slot_table)(targets)
    slot_token = slot_token + (jnp.arange(N_SP, dtype=jnp.int32) * TOK_SP)[:, None]
    table_tokens = jnp.transpose(slot_token.reshape(N_SP, EXPERTS, CAP), (1, 0, 2))
    table_live = jnp.transpose(slot_live.reshape(N_SP, EXPERTS, CAP), (1, 0, 2))
    ff_cols = EXPERT_FF // N_TP

    def one_expert(inputs):
        expert_id, token_ids, live_ids = inputs
        rows_in = jnp.where(live_ids[..., None] > 0, normed[token_ids], jnp.zeros((), jnp.bfloat16))
        flat_rows = rows_in.reshape(N_SP * CAP, D)
        gate_act = jnp.dot(flat_rows, gate_weight[expert_id], preferred_element_type=jnp.float32)
        up_act = jnp.dot(flat_rows, up_weight[expert_id], preferred_element_type=jnp.float32)
        hidden = (jax.nn.silu(gate_act) * up_act).astype(jnp.bfloat16)
        down_full = down_weight[expert_id]

        def add_part(group_index, running):
            first_col = (jnp.asarray(group_index) * ff_cols).astype(jnp.int32)
            piece = lax.dynamic_slice_in_dim(hidden, first_col, ff_cols, 1)
            weight_piece = lax.dynamic_slice_in_dim(down_full, first_col, ff_cols, 0)
            partial_value = jnp.dot(piece, weight_piece, preferred_element_type=jnp.float32).astype(jnp.bfloat16)
            return running + lax.optimization_barrier(partial_value).astype(jnp.float32)
        summed = lax.fori_loop(0, N_TP, add_part, jnp.zeros((N_SP * CAP, D), jnp.float32))
        return summed.reshape(N_SP, CAP, D)
    expert_out = lax.map(one_expert, (jnp.arange(EXPERTS, dtype=jnp.int32), table_tokens, table_live))
    by_block = jnp.transpose(expert_out, (1, 0, 2, 3)).reshape(N_SP, EXPERTS * CAP, D)
    picked = jnp.take_along_axis(by_block, targets[:, :, None], axis=1)
    weighted = picked * route_weights.astype(jnp.float32).reshape(N_SP, TOK_SP * TOPK)[:, :, None]
    moe = lax.optimization_barrier(jnp.sum(weighted.reshape(N_SP, TOK_SP, TOPK, D), axis=2)).reshape(TOKENS, D)
    return (stream.astype(jnp.float32) + moe).astype(jnp.bfloat16)
```

```python
import functools

import jax
import jax.numpy as jnp
from jax import lax
from jax.experimental import pallas as pl
from jax.experimental.pallas import tpu as pltpu
from jax.sharding import PartitionSpec as P

HEAD_DIM = 64
REP = 8
WINDOW = 128
MESH = pl.DeviceIdType.MESH

norm_eps = 1e-06


def shifted(block, axis, distance):
    devices = range(lax.axis_size(axis))
    route = [(i - distance, i) for i in devices if i - distance in devices]
    return lax.ppermute(block, axis, route)


def slot_targets(routes, experts_n, slot_cap):
    flat_ids = routes.reshape(-1)
    onehot = (flat_ids[:, None] == jnp.arange(experts_n, dtype=jnp.int32)[None, :]).astype(
        jnp.int32
    )
    before = jnp.cumsum(onehot, axis=0) - onehot
    targets = flat_ids * slot_cap + jnp.sum(before * onehot, axis=1)
    return targets.reshape(routes.shape)


def greet(n_sp, n_tp, sp, tp):
    barrier = pltpu.get_barrier_semaphore()
    for d in range(1, n_tp):
        pl.semaphore_signal(
            barrier, inc=1, device_id=(sp, lax.rem(tp + d, n_tp)), device_id_type=MESH
        )
    for d in range(1, n_sp):
        pl.semaphore_signal(
            barrier, inc=1, device_id=(lax.rem(sp + d, n_sp), tp), device_id_type=MESH
        )
    pl.semaphore_wait(barrier, n_tp + n_sp - 2)


def remote(src, dst, send, recv, device):
    return pltpu.make_async_remote_copy(
        src_ref=src,
        dst_ref=dst,
        send_sem=send,
        recv_sem=recv,
        device_id=device,
        device_id_type=MESH,
    )


def front_kernel(
    n_sp,
    n_tp,
    part,
    stream_in,
    gain,
    slots_row,
    arrived,
    stream_out,
    recv,
    squares,
    squares_in,
    outgoing,
    rs_send,
    rs_recv,
    sq_send,
    sq_recv,
    a2a_send,
    a2a_recv,
    ag_send,
    ag_recv,
):
    sp = lax.axis_index("sp")
    tp = lax.axis_index("tp")
    width = recv.shape[2]
    depth = part.shape[1]
    cap = arrived.shape[1]
    tok = part.shape[0]
    top = slots_row.shape[0]
    mine = pl.ds(pl.multiple_of(tp * width, width), width)
    greet(n_sp, n_tp, sp, tp)

    copies = []
    for d in range(1, n_tp):
        peer = lax.rem(tp + d, n_tp)
        cols = pl.ds(pl.multiple_of(peer * width, width), width)
        c = remote(
            part.at[:, cols], recv.at[d - 1], rs_send.at[d - 1], rs_recv.at[d - 1], (sp, peer)
        )
        c.start()
        copies.append(c)
    total = part[:, mine].astype(jnp.float32)
    for d in range(1, n_tp):
        copies[d - 1].wait_recv()
        total = total + recv[d - 1].astype(jnp.float32)
    stream = (stream_in[:, mine].astype(jnp.float32) + total).astype(jnp.bfloat16)
    stream_out[...] = stream
    values = stream.astype(jnp.float32)
    row_sum = jnp.sum(values * values, axis=1, keepdims=True)
    spread = jnp.transpose(jnp.broadcast_to(row_sum, (tok, 128)))
    squares[...] = spread[0:8]
    sq_copies = []
    for d in range(1, n_tp):
        peer = lax.rem(tp + d, n_tp)
        c = remote(squares, squares_in.at[d - 1], sq_send.at[d - 1], sq_recv.at[d - 1], (sp, peer))
        c.start()
        sq_copies.append(c)
    full = spread[0:8]
    for d in range(1, n_tp):
        sq_copies[d - 1].wait_recv()
        full = full + squares_in[d - 1]
    scale = lax.rsqrt(full / depth + norm_eps)
    scale = jnp.transpose(jnp.broadcast_to(scale[0:1], (128, tok)))[:, 0:1]
    normed = (values * scale * gain[:, mine]).astype(jnp.bfloat16)

    def picked(j):
        want = lax.broadcasted_iota(jnp.int32, (cap, tok), 0) + j * cap
        hit = want == slots_row[0:1, :]
        for k in range(1, top):
            hit = hit | (want == slots_row[k : k + 1, :])
        onehot = jnp.where(hit, 1.0, 0.0).astype(jnp.bfloat16)
        return jnp.dot(onehot, normed, preferred_element_type=jnp.float32).astype(jnp.bfloat16)

    a2a = []
    for d in range(1, n_sp):
        j = lax.rem(sp + d, n_sp)
        outgoing[d - 1] = picked(j)
        a2a.append(
            remote(
                outgoing.at[d - 1],
                arrived.at[sp, :, mine],
                a2a_send.at[d - 1],
                a2a_recv.at[d - 1],
                (j, tp),
            )
        )
        if d > 1:
            a2a[d - 2].start()
    arrived[sp, :, mine] = picked(sp)
    a2a[-1].start()
    gathers = []
    for d in range(n_sp):
        source = lax.rem(sp + n_sp - d, n_sp)
        if d > 0:
            a2a[d - 1].wait_recv()
        block = arrived.at[source, :, mine]
        for q in range(1, n_tp):
            peer = lax.rem(tp + q, n_tp)
            c = remote(block, block, ag_send.at[q - 1, d], ag_recv.at[q - 1, d], (sp, peer))
            c.start()
            gathers.append(c)
    for c in gathers:
        c.wait_recv()
    for c in copies + sq_copies + a2a + gathers:
        c.wait_send()


def back_kernel(
    n_sp,
    n_tp,
    part,
    slots,
    weights,
    stream,
    out,
    recv,
    summed,
    returned,
    joined,
    rs_send,
    rs_recv,
    a2a_send,
    a2a_recv,
    last_send,
    last_recv,
):
    sp = lax.axis_index("sp")
    tp = lax.axis_index("tp")
    width = recv.shape[3]
    cap = part.shape[1]
    tok = stream.shape[0]
    rows = out.shape[0]
    top = slots.shape[1]
    mine = pl.ds(pl.multiple_of(tp * width, width), width)
    greet(n_sp, n_tp, sp, tp)

    order = list(range(1, n_sp)) + [0]
    reduce = {}
    for d in order:
        s = lax.rem(sp + d, n_sp)
        for q in range(1, n_tp):
            peer = lax.rem(tp + q, n_tp)
            cols = pl.ds(pl.multiple_of(peer * width, width), width)
            c = remote(
                part.at[s, :, cols],
                recv.at[q - 1, d],
                rs_send.at[q - 1, d],
                rs_recv.at[q - 1, d],
                (sp, peer),
            )
            c.start()
            reduce[q, d] = c

    def added(d):
        s = lax.rem(sp + d, n_sp)
        total = part[s, :, mine].astype(jnp.float32)
        for q in range(1, n_tp):
            reduce[q, d].wait_recv()
            total = total + recv[q - 1, d].astype(jnp.float32)
        return total.astype(jnp.bfloat16)

    a2a = []
    for d in range(1, n_sp):
        s = lax.rem(sp + d, n_sp)
        summed[d - 1] = added(d)
        a2a.append(
            remote(
                summed.at[d - 1],
                returned.at[d - 1],
                a2a_send.at[d - 1],
                a2a_recv.at[d - 1],
                (s, tp),
            )
        )
        if d > 1:
            a2a[d - 2].start()
    a2a[-1].start()

    def taken(expert, block):
        want = lax.broadcasted_iota(jnp.int32, (tok, cap), 1) + expert * cap
        gives = None
        for k in range(top):
            onehot = jnp.where(want == slots[:, k : k + 1], 1.0, 0.0).astype(jnp.bfloat16)
            term = jnp.dot(onehot, block, preferred_element_type=jnp.float32)
            term = term * weights[:, k : k + 1]
            gives = term if gives is None else gives + term
        return gives

    moe = taken(sp, added(0))
    for d in range(1, n_sp):
        a2a[d - 1].wait_recv()
        moe = moe + taken(lax.rem(sp + n_sp - d, n_sp), returned[d - 1])
    joined[...] = (stream[...].astype(jnp.float32) + moe).astype(jnp.bfloat16)
    last = []
    for q in range(1, n_tp):
        peer = lax.rem(tp + q, n_tp)
        there = pl.ds(pl.multiple_of(peer * rows, rows), rows)
        c = remote(
            joined.at[there], out.at[:, mine], last_send.at[q - 1], last_recv.at[q - 1], (sp, peer)
        )
        c.start()
        last.append(c)
    out[:, mine] = joined[pl.ds(pl.multiple_of(tp * rows, rows), rows), :]
    for c in last:
        c.wait_recv()
    for c in list(reduce.values()) + a2a + last:
        c.wait_send()


def vmem(count):
    return [pl.BlockSpec(memory_space=pltpu.VMEM)] * count


def per_device(
    query_rows,
    key_rows,
    value_rows,
    sink_logits,
    out_weight,
    stream_in,
    norm_gain,
    routes,
    route_weights,
    gate_weight,
    up_weight,
    down_weight,
):
    n_sp = lax.axis_size("sp")
    n_tp = lax.axis_size("tp")
    tok_count = query_rows.shape[0]
    local_heads = query_rows.shape[1] // HEAD_DIM
    tp_index = lax.axis_index("tp")
    kv_group = tp_index * local_heads // REP
    own_keys = lax.dynamic_slice_in_dim(key_rows, kv_group * HEAD_DIM, HEAD_DIM, 1)
    own_values = lax.dynamic_slice_in_dim(value_rows, kv_group * HEAD_DIM, HEAD_DIM, 1)
    prior_keys, prior_values = shifted(
        (own_keys[tok_count - WINDOW :], own_values[tok_count - WINDOW :]), "sp", 1
    )
    key_block = jnp.concatenate([prior_keys, own_keys], axis=0)
    value_block = jnp.concatenate([prior_values, own_values], axis=0)
    offset = lax.axis_index("sp") * tok_count
    query_pos = offset + jnp.arange(tok_count, dtype=jnp.int32)
    key_pos = offset - WINDOW + jnp.arange(tok_count + WINDOW, dtype=jnp.int32)
    distance = query_pos[:, None] - key_pos[None, :]
    allowed = (distance >= 0) & (distance < WINDOW) & (key_pos >= 0)[None, :]
    queries = query_rows.reshape(tok_count, local_heads, HEAD_DIM)
    scores = jnp.einsum(
        "qhd,kd->hqk", queries, key_block, preferred_element_type=jnp.float32
    ) * HEAD_DIM ** (-0.5)
    scores = jnp.where(allowed[None], scores, -1e30)
    sink_col = sink_logits.reshape(local_heads, 1, 1)
    row_peak = jnp.maximum(jnp.max(scores, axis=-1, keepdims=True), sink_col)
    exp_terms = jnp.exp(scores - row_peak)
    denom_sum = jnp.sum(exp_terms, axis=-1, keepdims=True) + jnp.exp(sink_col - row_peak)
    attn_probs = (exp_terms / denom_sum).astype(jnp.bfloat16)
    attended = jnp.einsum(
        "hqk,kd->qhd", attn_probs, value_block, preferred_element_type=jnp.float32
    )
    attended = attended.astype(jnp.bfloat16).reshape(tok_count, local_heads * HEAD_DIM)
    projected = jnp.dot(attended, out_weight, preferred_element_type=jnp.float32).astype(
        jnp.bfloat16
    )

    depth = stream_in.shape[1]
    width = depth // n_tp
    row_share = tok_count // n_tp
    top_count = routes.shape[1]
    slot_cap = 3 * tok_count * top_count // (2 * n_sp)
    targets = slot_targets(routes, n_sp, slot_cap)
    bf16 = jnp.bfloat16
    dma = pltpu.SemaphoreType.DMA
    arrived, stream = pl.pallas_call(
        functools.partial(front_kernel, n_sp, n_tp),
        out_shape=(
            jax.ShapeDtypeStruct((n_sp, slot_cap, depth), bf16),
            jax.ShapeDtypeStruct((tok_count, width), bf16),
        ),
        in_specs=vmem(4),
        out_specs=tuple(vmem(2)),
        scratch_shapes=[
            pltpu.VMEM((n_tp - 1, tok_count, width), bf16),
            pltpu.VMEM((8, tok_count), jnp.float32),
            pltpu.VMEM((n_tp - 1, 8, tok_count), jnp.float32),
            pltpu.VMEM((n_sp - 1, slot_cap, width), bf16),
            dma((n_tp - 1,)),
            dma((n_tp - 1,)),
            dma((n_tp - 1,)),
            dma((n_tp - 1,)),
            dma((n_sp - 1,)),
            dma((n_sp - 1,)),
            dma((n_tp - 1, n_sp)),
            dma((n_tp - 1, n_sp)),
        ],
        compiler_params=pltpu.CompilerParams(
            collective_id=0, has_side_effects=True, vmem_limit_bytes=32 << 20
        ),
        name="front",
    )(projected, stream_in, norm_gain.reshape(1, depth), jnp.transpose(targets))
    flat_rows = arrived.reshape(n_sp * slot_cap, depth)
    gate_act = jnp.dot(flat_rows, gate_weight[0], preferred_element_type=jnp.float32)
    up_act = jnp.dot(flat_rows, up_weight[0], preferred_element_type=jnp.float32)
    hidden = (jax.nn.silu(gate_act) * up_act).astype(bf16)
    partial_value = jnp.dot(hidden, down_weight[0], preferred_element_type=jnp.float32).astype(bf16)
    partial_value = partial_value.reshape(n_sp, slot_cap, depth)
    return pl.pallas_call(
        functools.partial(back_kernel, n_sp, n_tp),
        out_shape=jax.ShapeDtypeStruct((row_share, depth), bf16),
        in_specs=vmem(4),
        out_specs=vmem(1)[0],
        scratch_shapes=[
            pltpu.VMEM((n_tp - 1, n_sp, slot_cap, width), bf16),
            pltpu.VMEM((n_sp - 1, slot_cap, width), bf16),
            pltpu.VMEM((n_sp - 1, slot_cap, width), bf16),
            pltpu.VMEM((tok_count, width), bf16),
            dma((n_tp - 1, n_sp)),
            dma((n_tp - 1, n_sp)),
            dma((n_sp - 1,)),
            dma((n_sp - 1,)),
            dma((n_tp - 1,)),
            dma((n_tp - 1,)),
        ],
        compiler_params=pltpu.CompilerParams(
            collective_id=1, has_side_effects=True, vmem_limit_bytes=32 << 20
        ),
        name="back",
    )(partial_value, targets, route_weights, stream)


def solution(mesh):
    return jax.shard_map(
        per_device,
        mesh=mesh,
        in_specs=(
            P("sp", "tp"),
            P("sp", None),
            P("sp", None),
            P("tp"),
            P("tp", None),
            P("sp", None),
            P(),
            P("sp", None),
            P("sp", None),
            P("sp", None, "tp"),
            P("sp", None, "tp"),
            P("sp", "tp", None),
        ),
        out_specs=P(("sp", "tp"), None),
        check_vma=False,
    )
```

```python
import functools

import jax
import jax.numpy as jnp
from jax import lax
from jax.experimental import pallas as pl
from jax.experimental.pallas import tpu as pltpu
from jax.sharding import PartitionSpec as P

HEAD_DIM = 64
REP = 8
WINDOW = 128
MESH = pl.DeviceIdType.MESH

norm_eps = 1e-06


def slot_targets(routes, experts_n, slot_cap):
    flat_ids = routes.reshape(-1)
    onehot = (flat_ids[:, None] == jnp.arange(experts_n, dtype=jnp.int32)[None, :]).astype(
        jnp.int32
    )
    before = jnp.cumsum(onehot, axis=0) - onehot
    targets = flat_ids * slot_cap + jnp.sum(before * onehot, axis=1)
    return targets.reshape(routes.shape)


def greet(n_sp, n_tp, sp, tp):
    barrier = pltpu.get_barrier_semaphore()
    for d in range(1, n_tp):
        pl.semaphore_signal(
            barrier, inc=1, device_id=(sp, lax.rem(tp + d, n_tp)), device_id_type=MESH
        )
    for d in range(1, n_sp):
        pl.semaphore_signal(
            barrier, inc=1, device_id=(lax.rem(sp + d, n_sp), tp), device_id_type=MESH
        )
    pl.semaphore_wait(barrier, n_tp + n_sp - 2)


def remote(src, dst, send, recv, device):
    return pltpu.make_async_remote_copy(
        src_ref=src,
        dst_ref=dst,
        send_sem=send,
        recv_sem=recv,
        device_id=device,
        device_id_type=MESH,
    )


GROUPS = 4


def layer_kernel(
    n_sp,
    n_tp,
    query,
    kv,
    sinks,
    gain,
    slots_row,
    slots,
    weights,
    out_w_hbm,
    stream_hbm,
    gate_hbm,
    up_hbm,
    down_hbm,
    out,
    halo,
    attended,
    out_w,
    stream_in,
    gate,
    up,
    down,
    part0,
    px0,
    py0,
    qx0,
    qy0,
    fx0,
    fy0,
    stream,
    squares,
    squares_in,
    outgoing,
    arrived,
    hidden,
    part,
    px,
    py,
    qx,
    qy,
    fx,
    fy,
    summed,
    returned,
    acc,
    joined,
    halo_sem,
    load_sem,
    rs_send,
    rs_recv,
    sq_send,
    sq_recv,
    a2a_send,
    a2a_recv,
    ag_send,
    ag_recv,
    ret_send,
    ret_recv,
    last_send,
    last_recv,
):
    sp = lax.axis_index("sp")
    tp = lax.axis_index("tp")
    relay = n_tp == 4
    tok, width = stream.shape
    depth = arrived.shape[2]
    cap = arrived.shape[1]
    top = slots.shape[1]
    rows = out.shape[0]
    size = n_sp // GROUPS
    half = width // 2
    ff = hidden.shape[1]
    across = tp + 1 - 2 * lax.rem(tp, 2)
    down_tp = lax.rem(tp + 2, n_tp)
    corner = lax.rem(across + 2, n_tp)
    f32 = jnp.float32
    bf16 = jnp.bfloat16

    def cols(p, part_of=None):
        if part_of is None:
            return pl.ds(pl.multiple_of(p * width, width), width)
        return pl.ds(pl.multiple_of(p * width + part_of * half, half), half)

    mine = cols(tp)
    loads = [
        pltpu.make_async_copy(out_w_hbm, out_w, load_sem.at[0]),
        pltpu.make_async_copy(stream_hbm.at[:, mine], stream_in, load_sem.at[1]),
        pltpu.make_async_copy(gate_hbm.at[0], gate, load_sem.at[2]),
        pltpu.make_async_copy(up_hbm.at[0], up, load_sem.at[3]),
        pltpu.make_async_copy(down_hbm.at[0], down, load_sem.at[4]),
    ]
    for c in loads:
        c.start()
    greet(n_sp, n_tp, sp, tp)
    sent = []

    def go(c):
        c.start()
        sent.append(c)
        return c

    tail = go(
        remote(
            kv.at[pl.ds(tok - WINDOW, WINDOW)],
            halo,
            halo_sem.at[0],
            halo_sem.at[1],
            (lax.rem(sp + 1, n_sp), tp),
        )
    )

    def reduce_first(src, lead, bufs, g):
        bx, by = bufs[0], bufs[1]
        pieces = []
        if relay:
            plan = (
                (1, corner, 0, bx.at[1], across),
                (3, corner, 1, by.at[1], down_tp),
                (0, across, 0, bx.at[0], across),
                (2, down_tp, 1, by.at[0], down_tp),
            )
            for i, owner, h, dst, to in plan:
                pieces.append(
                    go(
                        remote(
                            src.at[lead + (cols(owner, h),)],
                            dst,
                            rs_send.at[g, i],
                            rs_recv.at[g, i],
                            (sp, to),
                        )
                    )
                )
        else:
            for q in range(1, n_tp):
                peer = lax.rem(tp + q, n_tp)
                pieces.append(
                    go(
                        remote(
                            src.at[lead + (cols(peer),)],
                            bx.at[q - 1],
                            rs_send.at[g, q - 1],
                            rs_recv.at[g, q - 1],
                            (sp, peer),
                        )
                    )
                )
        return pieces

    def reduce_second(src, lead, bufs, g, pieces):
        if not relay:
            return
        bx, by, rx, ry, tx, ty = bufs
        pieces[0].wait_recv()
        ty[...] = (
            src[lead + (cols(down_tp, 0),)].astype(f32) + bx.at[1][...].astype(f32)
        ).astype(bf16)
        pieces[1].wait_recv()
        tx[...] = (
            src[lead + (cols(across, 1),)].astype(f32) + by.at[1][...].astype(f32)
        ).astype(bf16)
        pieces.append(go(remote(ty, ry, rs_send.at[g, 4], rs_recv.at[g, 4], (sp, down_tp))))
        pieces.append(go(remote(tx, rx, rs_send.at[g, 5], rs_recv.at[g, 5], (sp, across))))

    def reduce_last(src, lead, bufs, pieces):
        bx, by, rx, ry = bufs[:4]
        if not relay:
            total = src[lead + (mine,)].astype(f32)
            for q in range(1, n_tp):
                pieces[q - 1].wait_recv()
                total = total + bx.at[q - 1][...].astype(f32)
            return total
        pieces[2].wait_recv()
        pieces[4].wait_recv()
        first = src[lead + (cols(tp, 0),)].astype(f32) + bx.at[0][...].astype(f32)
        first = first + ry[...].astype(f32)
        pieces[3].wait_recv()
        pieces[5].wait_recv()
        second = src[lead + (cols(tp, 1),)].astype(f32) + by.at[0][...].astype(f32)
        second = second + rx[...].astype(f32)
        return jnp.concatenate([first, second], axis=-1)

    row_at = lax.broadcasted_iota(jnp.int32, (WINDOW, 2 * WINDOW), 0)
    col_at = lax.broadcasted_iota(jnp.int32, (WINDOW, 2 * WINDOW), 1)
    gap = row_at + WINDOW - col_at
    in_window = (gap >= 0) & (gap < WINDOW)
    blocks = list(range(1, tok // WINDOW)) + [0]
    for b in blocks:
        here = slice(b * WINDOW, (b + 1) * WINDOW)
        if b == 0:
            tail.wait_recv()
            prior = halo[...]
            allowed = in_window & (sp * tok - WINDOW + col_at >= 0)
        else:
            prior = kv[(b - 1) * WINDOW : b * WINDOW]
            allowed = in_window
        both = jnp.concatenate([prior, kv[here]], axis=0)
        keys, vals = both[:, :HEAD_DIM], both[:, HEAD_DIM:]
        for h in range(query.shape[1] // HEAD_DIM):
            lanes = slice(h * HEAD_DIM, (h + 1) * HEAD_DIM)
            scores = lax.dot_general(
                query[here, lanes], keys, (((1,), (1,)), ((), ())), preferred_element_type=f32
            ) * HEAD_DIM ** (-0.5)
            scores = jnp.where(allowed, scores, -1e30)
            sink = sinks[0:1, h : h + 1]
            peak = jnp.maximum(jnp.max(scores, axis=1, keepdims=True), sink)
            terms = jnp.exp(scores - peak)
            denom = jnp.sum(terms, axis=1, keepdims=True) + jnp.exp(sink - peak)
            probs = (terms / denom).astype(bf16)
            attended[here, lanes] = jnp.dot(probs, vals, preferred_element_type=f32).astype(bf16)
    loads[0].wait()
    for q in range(1, n_tp + 1):
        block = cols(lax.rem(tp + q, n_tp))
        part0[:, block] = jnp.dot(
            attended[...], out_w[:, block], preferred_element_type=f32
        ).astype(bf16)
    every = (slice(None),)
    bufs0 = (px0, py0, qx0, qy0, fx0, fy0)
    pieces = reduce_first(part0, every, bufs0, GROUPS)
    reduce_second(part0, every, bufs0, GROUPS, pieces)
    total = reduce_last(part0, every, bufs0, pieces)
    loads[1].wait()
    new_stream = (stream_in[...].astype(f32) + total).astype(bf16)
    values = new_stream.astype(f32)
    row_sum = jnp.sum(values * values, axis=1, keepdims=True)
    spread = jnp.transpose(jnp.broadcast_to(row_sum, (tok, 128)))
    squares[...] = spread[0:8]
    stream[...] = new_stream
    sq = []
    for d in range(1, n_tp):
        peer = lax.rem(tp + d, n_tp)
        sq.append(
            go(
                remote(
                    squares, squares_in.at[d - 1], sq_send.at[d - 1], sq_recv.at[d - 1], (sp, peer)
                )
            )
        )
    full = spread[0:8]
    for d in range(1, n_tp):
        sq[d - 1].wait_recv()
        full = full + squares_in[d - 1]
    scale = lax.rsqrt(full / depth + norm_eps)
    scale = jnp.transpose(jnp.broadcast_to(scale[0:1], (128, tok)))[:, 0:1]
    normed = (values * scale * gain[:, mine]).astype(bf16)

    def picked(j):
        want = lax.broadcasted_iota(jnp.int32, (cap, tok), 0) + j * cap
        hit = want == slots_row[0:1, :]
        for k in range(1, top):
            hit = hit | (want == slots_row[k : k + 1, :])
        onehot = jnp.where(hit, 1.0, 0.0).astype(bf16)
        return jnp.dot(onehot, normed, preferred_element_type=f32).astype(bf16)

    a2a = [None]
    for d in range(1, n_sp):
        j = lax.rem(sp + d, n_sp)
        outgoing[d - 1] = picked(j)
        a2a.append(
            remote(
                outgoing.at[d - 1],
                arrived.at[d, :, mine],
                a2a_send.at[d - 1],
                a2a_recv.at[d - 1],
                (j, tp),
            )
        )
        if d > 1:
            go(a2a[d - 1])
    arrived[0, :, mine] = picked(sp)
    go(a2a[-1])

    direct = {}

    def share(g, owner, part_of, i, to):
        block = arrived.at[pl.ds(g * size, size), :, cols(owner, part_of)]
        c = remote(block, block, ag_send.at[g, i], ag_recv.at[g, i], (sp, to))
        direct[g, i] = go(c)

    def gather_first(g):
        for d in range(g * size, (g + 1) * size):
            if d > 0:
                a2a[d].wait_recv()
        if relay:
            share(g, tp, None, 0, across)
            share(g, tp, None, 1, down_tp)
        else:
            for q in range(1, n_tp):
                share(g, tp, None, q - 1, lax.rem(tp + q, n_tp))

    def gather_second(g):
        if relay:
            direct[g, 0].wait_recv()
            share(g, across, 0, 2, down_tp)
            direct[g, 1].wait_recv()
            share(g, down_tp, 1, 3, across)

    def lead_of(g):
        return (pl.ds(g * size, size), slice(None))

    def bufs_of(g):
        return tuple(r.at[g] for r in (px, py, qx, qy, fx, fy))

    ff_tile = min(256, ff)

    def experts(g):
        for i in range(2 if relay else 0, 4 if relay else n_tp - 1):
            direct[g, i].wait_recv()
        if g == 0:
            for c in loads[2:]:
                c.wait()

        def inner(f, carry):
            lanes = pl.ds(pl.multiple_of(f * ff_tile, ff_tile), ff_tile)
            x = arrived[pl.ds(g * size, size)].reshape(size * cap, depth)
            gate_act = jnp.dot(x, gate[:, lanes], preferred_element_type=f32)
            up_act = jnp.dot(x, up[:, lanes], preferred_element_type=f32)
            hidden[:, lanes] = (jax.nn.silu(gate_act) * up_act).astype(bf16)
            return carry

        lax.fori_loop(0, ff // ff_tile, inner, 0)

        def outer(q, carry):
            block = cols(lax.rem(tp + 1 + q, n_tp))
            got = jnp.dot(hidden[...], down[:, block], preferred_element_type=f32).astype(bf16)
            part[pl.ds(g * size, size), :, block] = got.reshape(size, cap, width)
            return carry

        lax.fori_loop(0, n_tp, outer, 0)

    back = {}

    def send_back(g):
        total = reduce_last(part, lead_of(g), bufs_of(g), reduced[g]).astype(bf16)
        summed[pl.ds(g * size, size)] = total
        for d in range(g * size, (g + 1) * size):
            if d > 0:
                back[d] = go(
                    remote(
                        summed.at[d],
                        returned.at[d - 1],
                        ret_send.at[d - 1],
                        ret_recv.at[d - 1],
                        (lax.rem(sp + n_sp - d, n_sp), tp),
                    )
                )

    def take(g):
        for d in range(g * size, (g + 1) * size):
            if d > 0:
                back[d].wait_recv()
            block = returned[d - 1] if d > 0 else summed[0]
            expert = lax.rem(sp + d, n_sp)
            want = lax.broadcasted_iota(jnp.int32, (tok, cap), 1) + expert * cap
            gives = None if d == 0 else acc[...]
            for k in range(top):
                onehot = jnp.where(want == slots[:, k : k + 1], 1.0, 0.0).astype(bf16)
                term = jnp.dot(onehot, block, preferred_element_type=f32)
                term = term * weights[:, k : k + 1]
                gives = term if gives is None else gives + term
            acc[...] = gives

    reduced = {}
    for step in range(GROUPS + 5):
        if step < GROUPS:
            gather_first(step)
        if 1 <= step < GROUPS + 1:
            gather_second(step - 1)
        if 2 <= step < GROUPS + 2:
            g = step - 2
            experts(g)
            reduced[g] = reduce_first(part, lead_of(g), bufs_of(g), g)
        if 3 <= step < GROUPS + 3:
            g = step - 3
            reduce_second(part, lead_of(g), bufs_of(g), g, reduced[g])
        if 4 <= step < GROUPS + 4:
            send_back(step - 4)
        if 5 <= step:
            take(step - 5)

    joined[...] = (stream[...].astype(f32) + acc[...]).astype(bf16)
    last = []
    for q in range(1, n_tp):
        peer = lax.rem(tp + q, n_tp)
        there = pl.ds(pl.multiple_of(peer * rows, rows), rows)
        last.append(
            go(
                remote(
                    joined.at[there],
                    out.at[:, mine],
                    last_send.at[q - 1],
                    last_recv.at[q - 1],
                    (sp, peer),
                )
            )
        )
    out[:, mine] = joined[pl.ds(pl.multiple_of(tp * rows, rows), rows), :]
    for c in last:
        c.wait_recv()
    for c in sent:
        c.wait_send()


def vmem(count):
    return [pl.BlockSpec(memory_space=pltpu.VMEM)] * count


def per_device(
    query_rows,
    key_rows,
    value_rows,
    sink_logits,
    out_weight,
    stream_in,
    norm_gain,
    routes,
    route_weights,
    gate_weight,
    up_weight,
    down_weight,
):
    n_sp = lax.axis_size("sp")
    n_tp = lax.axis_size("tp")
    tok_count = query_rows.shape[0]
    local_heads = query_rows.shape[1] // HEAD_DIM
    tp_index = lax.axis_index("tp")
    kv_group = tp_index * local_heads // REP
    own_keys = lax.dynamic_slice_in_dim(key_rows, kv_group * HEAD_DIM, HEAD_DIM, 1)
    own_values = lax.dynamic_slice_in_dim(value_rows, kv_group * HEAD_DIM, HEAD_DIM, 1)
    kv = jnp.concatenate([own_keys, own_values], axis=1)
    depth = stream_in.shape[1]
    width = depth // n_tp
    half = width // 2
    row_share = tok_count // n_tp
    ff = gate_weight.shape[2]
    top_count = routes.shape[1]
    slot_cap = -(-3 * tok_count * top_count // (2 * n_sp) // 16) * 16
    targets = slot_targets(routes, n_sp, slot_cap)
    bf16 = jnp.bfloat16
    f32 = jnp.float32
    size = n_sp // GROUPS
    dma = pltpu.SemaphoreType.DMA
    buf = pltpu.VMEM
    if n_tp == 4:
        first0, first = (2, tok_count, half), (GROUPS, 2, size, slot_cap, half)
        second0, second = (tok_count, half), (GROUPS, size, slot_cap, half)
    else:
        first0 = (n_tp - 1, tok_count, width)
        first = (GROUPS, n_tp - 1, size, slot_cap, width)
        second0, second = (16, 128), (GROUPS, 16, 128)
    few = max(6, n_tp - 1)
    any_spec = pl.BlockSpec(memory_space=pl.ANY)
    return pl.pallas_call(
        functools.partial(layer_kernel, n_sp, n_tp),
        out_shape=jax.ShapeDtypeStruct((row_share, depth), bf16),
        in_specs=vmem(7) + [any_spec] * 5,
        out_specs=vmem(1)[0],
        scratch_shapes=[
            buf((WINDOW, 2 * HEAD_DIM), bf16),
            buf((tok_count, local_heads * HEAD_DIM), bf16),
            buf(out_weight.shape, bf16),
            buf((tok_count, width), bf16),
            buf((depth, ff), bf16),
            buf((depth, ff), bf16),
            buf((ff, depth), bf16),
            buf((tok_count, depth), bf16),
            buf(first0, bf16),
            buf(first0 if n_tp == 4 else second0, bf16),
            buf(second0, bf16),
            buf(second0, bf16),
            buf(second0, bf16),
            buf(second0, bf16),
            buf((tok_count, width), bf16),
            buf((8, tok_count), f32),
            buf((n_tp - 1, 8, tok_count), f32),
            buf((n_sp - 1, slot_cap, width), bf16),
            buf((n_sp, slot_cap, depth), bf16),
            buf((size * slot_cap, ff), bf16),
            buf((n_sp, slot_cap, depth), bf16),
            buf(first, bf16),
            buf(first if n_tp == 4 else second, bf16),
            buf(second, bf16),
            buf(second, bf16),
            buf(second, bf16),
            buf(second, bf16),
            buf((n_sp, slot_cap, width), bf16),
            buf((n_sp - 1, slot_cap, width), bf16),
            buf((tok_count, width), f32),
            buf((tok_count, width), bf16),
            dma((2,)),
            dma((5,)),
            dma((GROUPS + 1, few)),
            dma((GROUPS + 1, few)),
            dma((n_tp - 1,)),
            dma((n_tp - 1,)),
            dma((n_sp - 1,)),
            dma((n_sp - 1,)),
            dma((GROUPS, few)),
            dma((GROUPS, few)),
            dma((n_sp - 1,)),
            dma((n_sp - 1,)),
            dma((n_tp - 1,)),
            dma((n_tp - 1,)),
        ],
        compiler_params=pltpu.CompilerParams(
            collective_id=0, has_side_effects=True, vmem_limit_bytes=58 << 20
        ),
        name="layer",
    )(
        query_rows,
        kv,
        sink_logits.reshape(1, local_heads),
        norm_gain.reshape(1, depth),
        jnp.transpose(targets),
        targets,
        route_weights,
        out_weight,
        stream_in,
        gate_weight,
        up_weight,
        down_weight,
    )


def solution(mesh):
    return jax.shard_map(
        per_device,
        mesh=mesh,
        in_specs=(
            P("sp", "tp"),
            P("sp", None),
            P("sp", None),
            P("tp"),
            P("tp", None),
            P("sp", None),
            P(),
            P("sp", None),
            P("sp", None),
            P("sp", None, "tp"),
            P("sp", None, "tp"),
            P("sp", "tp", None),
        ),
        out_specs=P(("sp", "tp"), None),
        check_vma=False,
    )
```

```python
import functools

import jax
import jax.numpy as jnp
from jax import lax
from jax.experimental import pallas as pl
from jax.experimental.pallas import tpu as pltpu
from jax.sharding import PartitionSpec as P

HEAD_DIM = 64
REP = 8
WINDOW = 128
MESH = pl.DeviceIdType.MESH

norm_eps = 1e-06


def greet(n_sp, n_tp, sp, tp):
    barrier = pltpu.get_barrier_semaphore()
    for d in range(1, n_tp):
        pl.semaphore_signal(
            barrier, inc=1, device_id=(sp, lax.rem(tp + d, n_tp)), device_id_type=MESH
        )
    for d in range(1, n_sp):
        pl.semaphore_signal(
            barrier, inc=1, device_id=(lax.rem(sp + d, n_sp), tp), device_id_type=MESH
        )
    pl.semaphore_wait(barrier, n_tp + n_sp - 2)


def remote(src, dst, send, recv, device):
    return pltpu.make_async_remote_copy(
        src_ref=src,
        dst_ref=dst,
        send_sem=send,
        recv_sem=recv,
        device_id=device,
        device_id_type=MESH,
    )


GROUPS = 4


def layer_kernel(
    n_sp,
    n_tp,
    query,
    key_rows,
    value_rows,
    sinks,
    gain,
    routes,
    route_weights,
    out_w_hbm,
    stream_hbm,
    gate_hbm,
    up_hbm,
    down_hbm,
    out,
    halo,
    attended,
    out_w,
    stream_in,
    gate,
    up,
    down,
    part0,
    px0,
    py0,
    qx0,
    qy0,
    fx0,
    fy0,
    stream,
    squares,
    squares_in,
    outgoing,
    arrived,
    hidden,
    part,
    px,
    py,
    qx,
    qy,
    fx,
    fy,
    summed,
    returned,
    acc,
    joined,
    halo_sem,
    load_sem,
    rs_send,
    rs_recv,
    sq_send,
    sq_recv,
    a2a_send,
    a2a_recv,
    ag_send,
    ag_recv,
    ret_send,
    ret_recv,
    last_send,
    last_recv,
):
    sp = lax.axis_index("sp")
    tp = lax.axis_index("tp")
    relay = n_tp == 4
    tok, width = stream.shape
    depth = arrived.shape[2]
    cap = arrived.shape[1]
    top = routes.shape[0]
    rows = out.shape[0]
    size = n_sp // GROUPS
    half = width // 2
    ff = hidden.shape[1]
    across = tp + 1 - 2 * lax.rem(tp, 2)
    down_tp = lax.rem(tp + 2, n_tp)
    corner = lax.rem(across + 2, n_tp)
    f32 = jnp.float32
    bf16 = jnp.bfloat16

    def cols(p, part_of=None):
        if part_of is None:
            return pl.ds(pl.multiple_of(p * width, width), width)
        return pl.ds(pl.multiple_of(p * width + part_of * half, half), half)

    mine = cols(tp)
    loads = [
        pltpu.make_async_copy(out_w_hbm, out_w, load_sem.at[0]),
        pltpu.make_async_copy(stream_hbm.at[:, mine], stream_in, load_sem.at[1]),
        pltpu.make_async_copy(gate_hbm.at[0], gate, load_sem.at[2]),
        pltpu.make_async_copy(up_hbm.at[0], up, load_sem.at[3]),
        pltpu.make_async_copy(down_hbm.at[0], down, load_sem.at[4]),
    ]
    for c in loads:
        c.start()
    greet(n_sp, n_tp, sp, tp)
    sent = []

    def go(c):
        c.start()
        sent.append(c)
        return c

    local_heads = query.shape[1] // HEAD_DIM
    kv_group = tp * local_heads // REP
    pair = pl.ds(pl.multiple_of(kv_group // 2 * 2 * HEAD_DIM, 2 * HEAD_DIM), 2 * HEAD_DIM)
    odd = lax.rem(kv_group, 2) == 1
    tails = [
        go(
            remote(
                source.at[pl.ds(tok - WINDOW, WINDOW), pair],
                halo.at[i],
                halo_sem.at[0, i],
                halo_sem.at[1, i],
                (lax.rem(sp + 1, n_sp), tp),
            )
        )
        for i, source in enumerate((key_rows, value_rows))
    ]

    def reduce_first(src, lead, bufs, g):
        bx, by = bufs[0], bufs[1]
        pieces = []
        if relay:
            plan = (
                (1, corner, 0, bx.at[1], across),
                (3, corner, 1, by.at[1], down_tp),
                (0, across, 0, bx.at[0], across),
                (2, down_tp, 1, by.at[0], down_tp),
            )
            for i, owner, h, dst, to in plan:
                pieces.append(
                    go(
                        remote(
                            src.at[lead + (cols(owner, h),)],
                            dst,
                            rs_send.at[g, i],
                            rs_recv.at[g, i],
                            (sp, to),
                        )
                    )
                )
        else:
            for q in range(1, n_tp):
                peer = lax.rem(tp + q, n_tp)
                pieces.append(
                    go(
                        remote(
                            src.at[lead + (cols(peer),)],
                            bx.at[q - 1],
                            rs_send.at[g, q - 1],
                            rs_recv.at[g, q - 1],
                            (sp, peer),
                        )
                    )
                )
        return pieces

    def reduce_second(src, lead, bufs, g, pieces):
        if not relay:
            return
        bx, by, rx, ry, tx, ty = bufs
        pieces[0].wait_recv()
        ty[...] = (
            src[lead + (cols(down_tp, 0),)].astype(f32) + bx.at[1][...].astype(f32)
        ).astype(bf16)
        pieces[1].wait_recv()
        tx[...] = (
            src[lead + (cols(across, 1),)].astype(f32) + by.at[1][...].astype(f32)
        ).astype(bf16)
        pieces.append(go(remote(ty, ry, rs_send.at[g, 4], rs_recv.at[g, 4], (sp, down_tp))))
        pieces.append(go(remote(tx, rx, rs_send.at[g, 5], rs_recv.at[g, 5], (sp, across))))

    def reduce_last(src, lead, bufs, pieces):
        bx, by, rx, ry = bufs[:4]
        if not relay:
            total = src[lead + (mine,)].astype(f32)
            for q in range(1, n_tp):
                pieces[q - 1].wait_recv()
                total = total + bx.at[q - 1][...].astype(f32)
            return total
        pieces[2].wait_recv()
        pieces[4].wait_recv()
        first = src[lead + (cols(tp, 0),)].astype(f32) + bx.at[0][...].astype(f32)
        first = first + ry[...].astype(f32)
        pieces[3].wait_recv()
        pieces[5].wait_recv()
        second = src[lead + (cols(tp, 1),)].astype(f32) + by.at[0][...].astype(f32)
        second = second + rx[...].astype(f32)
        return jnp.concatenate([first, second], axis=-1)

    def lead0(b):
        return (pl.ds(b * WINDOW, WINDOW),)

    def bufs0(b):
        return tuple(ref.at[b] for ref in (px0, py0, qx0, qy0, fx0, fy0))

    row_at = lax.broadcasted_iota(jnp.int32, (WINDOW, 2 * WINDOW), 0)
    col_at = lax.broadcasted_iota(jnp.int32, (WINDOW, 2 * WINDOW), 1)
    gap = row_at + WINDOW - col_at
    in_window = (gap >= 0) & (gap < WINDOW)

    def own_head(both):
        return jnp.where(odd, both[:, HEAD_DIM:], both[:, :HEAD_DIM])

    begun = {}
    waited = False
    blocks = list(range(1, tok // WINDOW)) + [0]
    for b in blocks:
        here = slice(b * WINDOW, (b + 1) * WINDOW)
        if b == 0:
            for c in tails:
                c.wait_recv()
            priors = (halo[0], halo[1])
            allowed = in_window & (sp * tok - WINDOW + col_at >= 0)
        else:
            before = slice((b - 1) * WINDOW, b * WINDOW)
            priors = (key_rows[before, pair], value_rows[before, pair])
            allowed = in_window
        keys, vals = (
            own_head(jnp.concatenate([prior, source[here, pair]], axis=0))
            for prior, source in zip(priors, (key_rows, value_rows))
        )
        for h in range(local_heads):
            lanes = slice(h * HEAD_DIM, (h + 1) * HEAD_DIM)
            scores = lax.dot_general(
                query[here, lanes], keys, (((1,), (1,)), ((), ())), preferred_element_type=f32
            ) * HEAD_DIM ** (-0.5)
            scores = jnp.where(allowed, scores, -1e30)
            sink = sinks[0:1, h : h + 1]
            peak = jnp.maximum(jnp.max(scores, axis=1, keepdims=True), sink)
            terms = jnp.exp(scores - peak)
            denom = jnp.sum(terms, axis=1, keepdims=True) + jnp.exp(sink - peak)
            probs = (terms / denom).astype(bf16)
            attended[here, lanes] = jnp.dot(probs, vals, preferred_element_type=f32).astype(bf16)
        if not waited:
            loads[0].wait()
            waited = True
        for q in range(1, n_tp + 1):
            block = cols(lax.rem(tp + q, n_tp))
            part0[here, block] = jnp.dot(
                attended[here], out_w[:, block], preferred_element_type=f32
            ).astype(bf16)
        begun[b] = reduce_first(part0, lead0(b), bufs0(b), n_sp + b)

    expert_at = lax.broadcasted_iota(jnp.int32, (n_sp, tok), 0)
    members = [
        jnp.where(routes[k : k + 1, :] == expert_at, 1.0, 0.0).astype(f32) for k in range(top)
    ]
    earlier = jnp.where(
        lax.broadcasted_iota(jnp.int32, (tok, tok), 0)
        < lax.broadcasted_iota(jnp.int32, (tok, tok), 1),
        1.0,
        0.0,
    ).astype(bf16)
    rank = jnp.dot(sum(members).astype(bf16), earlier, preferred_element_type=f32)
    slots_row = [
        routes[k : k + 1, :].astype(f32) * cap
        + jnp.sum(rank * members[k], axis=0, keepdims=True)
        for k in range(top)
    ]

    def upright(row):
        return jnp.transpose(jnp.broadcast_to(row, (128, tok)))[:, 0:1]

    slots = [upright(row) for row in slots_row]
    weights = [upright(route_weights[k : k + 1, :]) for k in range(top)]

    for b in blocks:
        reduce_second(part0, lead0(b), bufs0(b), n_sp + b, begun[b])
    total = jnp.concatenate(
        [reduce_last(part0, lead0(b), bufs0(b), begun[b]) for b in sorted(blocks)], axis=0
    )
    loads[1].wait()
    new_stream = (stream_in[...].astype(f32) + total).astype(bf16)
    values = new_stream.astype(f32)
    row_sum = jnp.sum(values * values, axis=1, keepdims=True)
    spread = jnp.transpose(jnp.broadcast_to(row_sum, (tok, 128)))
    squares[...] = spread[0:8]
    stream[...] = new_stream
    sq = []
    for d in range(1, n_tp):
        peer = lax.rem(tp + d, n_tp)
        sq.append(
            go(
                remote(
                    squares, squares_in.at[d - 1], sq_send.at[d - 1], sq_recv.at[d - 1], (sp, peer)
                )
            )
        )
    full = spread[0:8]
    for d in range(1, n_tp):
        sq[d - 1].wait_recv()
        full = full + squares_in[d - 1]
    scale = lax.rsqrt(full / depth + norm_eps)
    scale = upright(scale[0:1])
    normed = (values * scale * gain[:, mine]).astype(bf16)

    def picked(j):
        want = (lax.broadcasted_iota(jnp.int32, (cap, tok), 0) + j * cap).astype(f32)
        hit = want == slots_row[0]
        for k in range(1, top):
            hit = hit | (want == slots_row[k])
        onehot = jnp.where(hit, 1.0, 0.0).astype(bf16)
        return jnp.dot(onehot, normed, preferred_element_type=f32).astype(bf16)

    direct = {}

    def share(d, owner, part_of, i, to):
        block = arrived.at[d, :, cols(owner, part_of)]
        c = remote(block, block, ag_send.at[d, i], ag_recv.at[d, i], (sp, to))
        direct[d, i] = go(c)

    def gather_first(d):
        if d > 0:
            a2a[d].wait_recv()
        if relay:
            share(d, tp, None, 0, across)
            share(d, tp, None, 1, down_tp)
        else:
            for q in range(1, n_tp):
                share(d, tp, None, q - 1, lax.rem(tp + q, n_tp))

    def gather_second(d):
        if relay:
            direct[d, 0].wait_recv()
            share(d, across, 0, 2, down_tp)
            direct[d, 1].wait_recv()
            share(d, down_tp, 1, 3, across)

    def group(g):
        return range(g * size, (g + 1) * size)

    arrived[0, :, mine] = picked(sp)
    a2a = [None]
    for d in range(1, n_sp):
        j = lax.rem(sp + d, n_sp)
        outgoing[d - 1] = picked(j)
        a2a.append(
            remote(
                outgoing.at[d - 1],
                arrived.at[d, :, mine],
                a2a_send.at[d - 1],
                a2a_recv.at[d - 1],
                (j, tp),
            )
        )
        if d > 1:
            go(a2a[d - 1])
        if d == 2:
            gather_first(0)
    go(a2a[-1])

    def lead_of(g):
        return (g, slice(None))

    def bufs_of(g):
        return tuple(r.at[g] for r in (px, py, qx, qy, fx, fy))

    ff_tile = min(256, ff)

    def experts(g):
        for d in group(g):
            for i in range(2 if relay else 0, 4 if relay else n_tp - 1):
                direct[d, i].wait_recv()
        if g == 0:
            for c in loads[2:]:
                c.wait()

        def inner(f, carry):
            lanes = pl.ds(pl.multiple_of(f * ff_tile, ff_tile), ff_tile)
            x = arrived[pl.ds(g * size, size)].reshape(size * cap, depth)
            gate_act = jnp.dot(x, gate[:, lanes], preferred_element_type=f32)
            up_act = jnp.dot(x, up[:, lanes], preferred_element_type=f32)
            hidden[:, lanes] = (jax.nn.silu(gate_act) * up_act).astype(bf16)
            return carry

        lax.fori_loop(0, ff // ff_tile, inner, 0)

        def outer(q, carry):
            block = cols(lax.rem(tp + 1 + q, n_tp))
            got = jnp.dot(hidden[...], down[:, block], preferred_element_type=f32).astype(bf16)
            part[pl.ds(g * size, size), :, block] = got.reshape(size, cap, width)
            return carry

        lax.fori_loop(0, n_tp, outer, 0)

    back = {}

    def send_back(d):
        total = reduce_last(part, lead_of(d), bufs_of(d), reduced[d])
        summed[d] = total.astype(bf16)
        if d > 0:
            back[d] = go(
                remote(
                    summed.at[d],
                    returned.at[d - 1],
                    ret_send.at[d - 1],
                    ret_recv.at[d - 1],
                    (lax.rem(sp + n_sp - d, n_sp), tp),
                )
            )

    def take(g):
        for d in group(g):
            if d > 0:
                back[d].wait_recv()
            block = returned[d - 1] if d > 0 else summed[0]
            expert = lax.rem(sp + d, n_sp)
            want = (lax.broadcasted_iota(jnp.int32, (tok, cap), 1) + expert * cap).astype(f32)
            gives = None if d == 0 else acc[...]
            for k in range(top):
                onehot = jnp.where(want == slots[k], 1.0, 0.0).astype(bf16)
                term = jnp.dot(onehot, block, preferred_element_type=f32)
                term = term * weights[k]
                gives = term if gives is None else gives + term
            acc[...] = gives

    reduced = {}
    for step in range(GROUPS + 5):
        if step < GROUPS:
            for d in group(step):
                if d > 0:
                    gather_first(d)
        if 1 <= step < GROUPS + 1:
            for d in group(step - 1):
                gather_second(d)
        if 2 <= step < GROUPS + 2:
            experts(step - 2)
            for d in group(step - 2):
                reduced[d] = reduce_first(part, lead_of(d), bufs_of(d), d)
        if 3 <= step < GROUPS + 3:
            for d in group(step - 3):
                reduce_second(part, lead_of(d), bufs_of(d), d, reduced[d])
        if 4 <= step < GROUPS + 4:
            for d in group(step - 4):
                send_back(d)
        if 5 <= step:
            take(step - 5)

    joined[...] = (stream[...].astype(f32) + acc[...]).astype(bf16)
    last = []
    for q in range(1, n_tp):
        peer = lax.rem(tp + q, n_tp)
        there = pl.ds(pl.multiple_of(peer * rows, rows), rows)
        last.append(
            go(
                remote(
                    joined.at[there],
                    out.at[:, mine],
                    last_send.at[q - 1],
                    last_recv.at[q - 1],
                    (sp, peer),
                )
            )
        )
    out[:, mine] = joined[pl.ds(pl.multiple_of(tp * rows, rows), rows), :]
    for c in last:
        c.wait_recv()
    for c in sent:
        c.wait_send()


def vmem(count):
    return [pl.BlockSpec(memory_space=pltpu.VMEM)] * count


def per_device(
    query_rows,
    key_rows,
    value_rows,
    sink_logits,
    out_weight,
    stream_in,
    norm_gain,
    routes,
    route_weights,
    gate_weight,
    up_weight,
    down_weight,
):
    n_sp = lax.axis_size("sp")
    n_tp = lax.axis_size("tp")
    tok_count = query_rows.shape[0]
    local_heads = query_rows.shape[1] // HEAD_DIM
    depth = stream_in.shape[1]
    width = depth // n_tp
    half = width // 2
    row_share = tok_count // n_tp
    ff = gate_weight.shape[2]
    top_count = routes.shape[1]
    slot_cap = -(-3 * tok_count * top_count // (2 * n_sp) // 16) * 16
    bf16 = jnp.bfloat16
    f32 = jnp.float32
    size = n_sp // GROUPS
    blocks = tok_count // WINDOW
    dma = pltpu.SemaphoreType.DMA
    buf = pltpu.VMEM
    if n_tp == 4:
        first0, first = (blocks, 2, WINDOW, half), (n_sp, 2, slot_cap, half)
        second0, second = (blocks, WINDOW, half), (n_sp, slot_cap, half)
    else:
        first0 = (blocks, n_tp - 1, WINDOW, width)
        first = (n_sp, n_tp - 1, slot_cap, width)
        second0, second = (blocks, 16, 128), (n_sp, 16, 128)
    few = max(6, n_tp - 1)
    any_spec = pl.BlockSpec(memory_space=pl.ANY)
    return pl.pallas_call(
        functools.partial(layer_kernel, n_sp, n_tp),
        out_shape=jax.ShapeDtypeStruct((row_share, depth), bf16),
        in_specs=vmem(7) + [any_spec] * 5,
        out_specs=vmem(1)[0],
        scratch_shapes=[
            buf((2, WINDOW, 2 * HEAD_DIM), bf16),
            buf((tok_count, local_heads * HEAD_DIM), bf16),
            buf(out_weight.shape, bf16),
            buf((tok_count, width), bf16),
            buf((depth, ff), bf16),
            buf((depth, ff), bf16),
            buf((ff, depth), bf16),
            buf((tok_count, depth), bf16),
            buf(first0, bf16),
            buf(first0 if n_tp == 4 else second0, bf16),
            buf(second0, bf16),
            buf(second0, bf16),
            buf(second0, bf16),
            buf(second0, bf16),
            buf((tok_count, width), bf16),
            buf((8, tok_count), f32),
            buf((n_tp - 1, 8, tok_count), f32),
            buf((n_sp - 1, slot_cap, width), bf16),
            buf((n_sp, slot_cap, depth), bf16),
            buf((size * slot_cap, ff), bf16),
            buf((n_sp, slot_cap, depth), bf16),
            buf(first, bf16),
            buf(first if n_tp == 4 else second, bf16),
            buf(second, bf16),
            buf(second, bf16),
            buf(second, bf16),
            buf(second, bf16),
            buf((n_sp, slot_cap, width), bf16),
            buf((n_sp - 1, slot_cap, width), bf16),
            buf((tok_count, width), f32),
            buf((tok_count, width), bf16),
            dma((2, 2)),
            dma((5,)),
            dma((n_sp + blocks, few)),
            dma((n_sp + blocks, few)),
            dma((n_tp - 1,)),
            dma((n_tp - 1,)),
            dma((n_sp - 1,)),
            dma((n_sp - 1,)),
            dma((n_sp, few)),
            dma((n_sp, few)),
            dma((n_sp - 1,)),
            dma((n_sp - 1,)),
            dma((n_tp - 1,)),
            dma((n_tp - 1,)),
        ],
        compiler_params=pltpu.CompilerParams(
            collective_id=0, has_side_effects=True, vmem_limit_bytes=58 << 20
        ),
        name="layer",
    )(
        query_rows,
        key_rows,
        value_rows,
        sink_logits.reshape(1, local_heads),
        norm_gain.reshape(1, depth),
        jnp.transpose(routes),
        jnp.transpose(route_weights),
        out_weight,
        stream_in,
        gate_weight,
        up_weight,
        down_weight,
    )


def solution(mesh):
    return jax.shard_map(
        per_device,
        mesh=mesh,
        in_specs=(
            P("sp", "tp"),
            P("sp", None),
            P("sp", None),
            P("tp"),
            P("tp", None),
            P("sp", None),
            P(),
            P("sp", None),
            P("sp", None),
            P("sp", None, "tp"),
            P("sp", None, "tp"),
            P("sp", "tp", None),
        ),
        out_specs=P(("sp", "tp"), None),
        check_vma=False,
    )
```

```python
import functools

import jax
import jax.numpy as jnp
from jax import lax
from jax.experimental import pallas as pl
from jax.experimental.pallas import tpu as pltpu
from jax.sharding import PartitionSpec as P

HEAD_DIM = 64
REP = 8
WINDOW = 128
MESH = pl.DeviceIdType.MESH

norm_eps = 1e-06


def greet(n_sp, n_tp, sp, tp):
    barrier = pltpu.get_barrier_semaphore()
    for d in range(1, n_tp):
        pl.semaphore_signal(
            barrier, inc=1, device_id=(sp, lax.rem(tp + d, n_tp)), device_id_type=MESH
        )
    for d in range(1, n_sp):
        pl.semaphore_signal(
            barrier, inc=1, device_id=(lax.rem(sp + d, n_sp), tp), device_id_type=MESH
        )
    pl.semaphore_wait(barrier, n_tp + n_sp - 2)


def remote(src, dst, send, recv, device):
    return pltpu.make_async_remote_copy(
        src_ref=src,
        dst_ref=dst,
        send_sem=send,
        recv_sem=recv,
        device_id=device,
        device_id_type=MESH,
    )


GROUPS = 4


def layer_kernel(
    n_sp,
    n_tp,
    query,
    key_rows,
    value_rows,
    sinks,
    gain,
    routes,
    route_weights,
    out_w_hbm,
    stream_hbm,
    gate_hbm,
    up_hbm,
    down_hbm,
    out,
    halo,
    attended,
    out_w,
    stream_in,
    gate,
    up,
    down,
    part0,
    px0,
    py0,
    qx0,
    qy0,
    fx0,
    fy0,
    stream,
    squares,
    squares_in,
    outgoing,
    arrived,
    hidden,
    part,
    px,
    py,
    qx,
    qy,
    fx,
    fy,
    summed,
    returned,
    acc,
    joined,
    halo_sem,
    load_sem,
    rs_send,
    rs_recv,
    sq_send,
    sq_recv,
    a2a_send,
    a2a_recv,
    ag_send,
    ag_recv,
    ret_send,
    ret_recv,
    last_send,
    last_recv,
):
    sp = lax.axis_index("sp")
    tp = lax.axis_index("tp")
    relay = n_tp == 4
    tok, width = stream.shape
    depth = arrived.shape[2]
    cap = arrived.shape[1]
    top = routes.shape[0]
    rows = out.shape[0]
    size = n_sp // GROUPS
    half = width // 2
    ff = hidden.shape[1]
    across = tp + 1 - 2 * lax.rem(tp, 2)
    down_tp = lax.rem(tp + 2, n_tp)
    corner = lax.rem(across + 2, n_tp)
    f32 = jnp.float32
    bf16 = jnp.bfloat16

    def cols(p, part_of=None):
        if part_of is None:
            return pl.ds(pl.multiple_of(p * width, width), width)
        return pl.ds(pl.multiple_of(p * width + part_of * half, half), half)

    mine = cols(tp)
    loads = [
        pltpu.make_async_copy(out_w_hbm, out_w, load_sem.at[0]),
        pltpu.make_async_copy(stream_hbm.at[:, mine], stream_in, load_sem.at[1]),
        pltpu.make_async_copy(gate_hbm.at[0], gate, load_sem.at[2]),
        pltpu.make_async_copy(up_hbm.at[0], up, load_sem.at[3]),
        pltpu.make_async_copy(down_hbm.at[0], down, load_sem.at[4]),
    ]
    for c in loads:
        c.start()
    greet(n_sp, n_tp, sp, tp)
    sent = []

    def go(c):
        c.start()
        sent.append(c)
        return c

    local_heads = query.shape[1] // HEAD_DIM
    kv_group = tp * local_heads // REP
    pair = pl.ds(pl.multiple_of(kv_group // 2 * 2 * HEAD_DIM, 2 * HEAD_DIM), 2 * HEAD_DIM)
    odd = lax.rem(kv_group, 2) == 1
    tails = [
        go(
            remote(
                source.at[pl.ds(tok - WINDOW, WINDOW), pair],
                halo.at[i],
                halo_sem.at[0, i],
                halo_sem.at[1, i],
                (lax.rem(sp + 1, n_sp), tp),
            )
        )
        for i, source in enumerate((key_rows, value_rows))
    ]

    def reduce_first(src, lead, bufs, g):
        bx, by = bufs[0], bufs[1]
        pieces = []
        if relay:
            plan = (
                (1, corner, 0, bx.at[1], across),
                (3, corner, 1, by.at[1], down_tp),
                (0, across, 0, bx.at[0], across),
                (2, down_tp, 1, by.at[0], down_tp),
            )
            for i, owner, h, dst, to in plan:
                pieces.append(
                    go(
                        remote(
                            src.at[lead + (cols(owner, h),)],
                            dst,
                            rs_send.at[g, i],
                            rs_recv.at[g, i],
                            (sp, to),
                        )
                    )
                )
        else:
            for q in range(1, n_tp):
                peer = lax.rem(tp + q, n_tp)
                pieces.append(
                    go(
                        remote(
                            src.at[lead + (cols(peer),)],
                            bx.at[q - 1],
                            rs_send.at[g, q - 1],
                            rs_recv.at[g, q - 1],
                            (sp, peer),
                        )
                    )
                )
        return pieces

    def reduce_second(src, lead, bufs, g, pieces):
        if not relay:
            return
        bx, by, rx, ry, tx, ty = bufs
        pieces[0].wait_recv()
        ty[...] = (
            src[lead + (cols(down_tp, 0),)].astype(f32) + bx.at[1][...].astype(f32)
        ).astype(bf16)
        pieces[1].wait_recv()
        tx[...] = (
            src[lead + (cols(across, 1),)].astype(f32) + by.at[1][...].astype(f32)
        ).astype(bf16)
        pieces.append(go(remote(ty, ry, rs_send.at[g, 4], rs_recv.at[g, 4], (sp, down_tp))))
        pieces.append(go(remote(tx, rx, rs_send.at[g, 5], rs_recv.at[g, 5], (sp, across))))

    def reduce_last(src, lead, bufs, pieces):
        bx, by, rx, ry = bufs[:4]
        if not relay:
            total = src[lead + (mine,)].astype(f32)
            for q in range(1, n_tp):
                pieces[q - 1].wait_recv()
                total = total + bx.at[q - 1][...].astype(f32)
            return total
        pieces[2].wait_recv()
        pieces[4].wait_recv()
        first = src[lead + (cols(tp, 0),)].astype(f32) + bx.at[0][...].astype(f32)
        first = first + ry[...].astype(f32)
        pieces[3].wait_recv()
        pieces[5].wait_recv()
        second = src[lead + (cols(tp, 1),)].astype(f32) + by.at[0][...].astype(f32)
        second = second + rx[...].astype(f32)
        return jnp.concatenate([first, second], axis=-1)

    def lead0(b):
        return (pl.ds(b * WINDOW, WINDOW),)

    def bufs0(b):
        return tuple(ref.at[b] for ref in (px0, py0, qx0, qy0, fx0, fy0))

    row_at = lax.broadcasted_iota(jnp.int32, (WINDOW, 2 * WINDOW), 0)
    col_at = lax.broadcasted_iota(jnp.int32, (WINDOW, 2 * WINDOW), 1)
    gap = row_at + WINDOW - col_at
    in_window = (gap >= 0) & (gap < WINDOW)

    def own_head(both):
        return jnp.where(odd, both[:, HEAD_DIM:], both[:, :HEAD_DIM])

    begun = {}
    waited = False
    blocks = list(range(1, tok // WINDOW)) + [0]
    for b in blocks:
        here = slice(b * WINDOW, (b + 1) * WINDOW)
        if b == 0:
            for c in tails:
                c.wait_recv()
            priors = (halo[0], halo[1])
            allowed = in_window & (sp * tok - WINDOW + col_at >= 0)
        else:
            before = slice((b - 1) * WINDOW, b * WINDOW)
            priors = (key_rows[before, pair], value_rows[before, pair])
            allowed = in_window
        keys, vals = (
            own_head(jnp.concatenate([prior, source[here, pair]], axis=0))
            for prior, source in zip(priors, (key_rows, value_rows))
        )
        for h in range(local_heads):
            lanes = slice(h * HEAD_DIM, (h + 1) * HEAD_DIM)
            scores = lax.dot_general(
                query[here, lanes], keys, (((1,), (1,)), ((), ())), preferred_element_type=f32
            ) * HEAD_DIM ** (-0.5)
            scores = jnp.where(allowed, scores, -1e30)
            sink = sinks[0:1, h : h + 1]
            peak = jnp.maximum(jnp.max(scores, axis=1, keepdims=True), sink)
            terms = jnp.exp(scores - peak)
            denom = jnp.sum(terms, axis=1, keepdims=True) + jnp.exp(sink - peak)
            probs = (terms / denom).astype(bf16)
            attended[here, lanes] = jnp.dot(probs, vals, preferred_element_type=f32).astype(bf16)
        if not waited:
            loads[0].wait()
            waited = True
        for q in range(1, n_tp + 1):
            block = cols(lax.rem(tp + q, n_tp))
            part0[here, block] = jnp.dot(
                attended[here], out_w[:, block], preferred_element_type=f32
            ).astype(bf16)
        begun[b] = reduce_first(part0, lead0(b), bufs0(b), n_sp + b)

    expert_at = lax.broadcasted_iota(jnp.int32, (n_sp, tok), 0)
    members = [
        jnp.where(routes[k : k + 1, :] == expert_at, 1.0, 0.0).astype(f32) for k in range(top)
    ]
    earlier = jnp.where(
        lax.broadcasted_iota(jnp.int32, (tok, tok), 0)
        < lax.broadcasted_iota(jnp.int32, (tok, tok), 1),
        1.0,
        0.0,
    ).astype(bf16)
    rank = jnp.dot(sum(members).astype(bf16), earlier, preferred_element_type=f32)
    slots_row = [
        routes[k : k + 1, :].astype(f32) * cap
        + jnp.sum(rank * members[k], axis=0, keepdims=True)
        for k in range(top)
    ]

    def upright(row):
        return jnp.transpose(jnp.broadcast_to(row, (128, tok)))[:, 0:1]

    slots = [upright(row) for row in slots_row]
    weights = [upright(route_weights[k : k + 1, :]) for k in range(top)]

    for b in blocks:
        reduce_second(part0, lead0(b), bufs0(b), n_sp + b, begun[b])
    total = jnp.concatenate(
        [reduce_last(part0, lead0(b), bufs0(b), begun[b]) for b in sorted(blocks)], axis=0
    )
    loads[1].wait()
    new_stream = (stream_in[...].astype(f32) + total).astype(bf16)
    values = new_stream.astype(f32)
    row_sum = jnp.sum(values * values, axis=1, keepdims=True)
    spread = jnp.transpose(jnp.broadcast_to(row_sum, (tok, 128)))
    squares[...] = spread[0:8]
    stream[...] = new_stream
    sq = []
    for d in range(1, n_tp):
        peer = lax.rem(tp + d, n_tp)
        sq.append(
            go(
                remote(
                    squares, squares_in.at[d - 1], sq_send.at[d - 1], sq_recv.at[d - 1], (sp, peer)
                )
            )
        )
    full = spread[0:8]
    for d in range(1, n_tp):
        sq[d - 1].wait_recv()
        full = full + squares_in[d - 1]
    scale = lax.rsqrt(full / depth + norm_eps)
    scale = upright(scale[0:1])
    normed = (values * scale * gain[:, mine]).astype(bf16)

    def picked(j):
        want = (lax.broadcasted_iota(jnp.int32, (cap, tok), 0) + j * cap).astype(f32)
        hit = want == slots_row[0]
        for k in range(1, top):
            hit = hit | (want == slots_row[k])
        onehot = jnp.where(hit, 1.0, 0.0).astype(bf16)
        return jnp.dot(onehot, normed, preferred_element_type=f32).astype(bf16)

    direct = {}

    def share(d, owner, part_of, i, to):
        block = arrived.at[d, :, cols(owner, part_of)]
        c = remote(block, block, ag_send.at[d, i], ag_recv.at[d, i], (sp, to))
        direct[d, i] = go(c)

    def gather_first(d):
        if d > 0:
            a2a[d].wait_recv()
        if relay:
            share(d, tp, None, 0, across)
            share(d, tp, None, 1, down_tp)
        else:
            for q in range(1, n_tp):
                share(d, tp, None, q - 1, lax.rem(tp + q, n_tp))

    def gather_second(d):
        if relay:
            direct[d, 0].wait_recv()
            share(d, across, 0, 2, down_tp)
            direct[d, 1].wait_recv()
            share(d, down_tp, 1, 3, across)

    def group(g):
        return range(g * size, (g + 1) * size)

    reach = [0, 1, n_sp - 1]
    reach += sorted(range(2, n_sp - 1), key=lambda d: -min(d, n_sp - d))
    arrived[0, :, mine] = picked(sp)
    a2a = [None]
    for d in range(1, n_sp):
        j = lax.rem(sp + reach[d], n_sp)
        outgoing[d - 1] = picked(j)
        a2a.append(
            remote(
                outgoing.at[d - 1],
                arrived.at[d, :, mine],
                a2a_send.at[d - 1],
                a2a_recv.at[d - 1],
                (j, tp),
            )
        )
        if d > 1:
            go(a2a[d - 1])
        if d == 2:
            gather_first(0)
    go(a2a[-1])

    def lead_of(g):
        return (g, slice(None))

    def bufs_of(g):
        return tuple(r.at[g] for r in (px, py, qx, qy, fx, fy))

    ff_tile = min(256, ff)

    def experts(g):
        for d in group(g):
            for i in range(2 if relay else 0, 4 if relay else n_tp - 1):
                direct[d, i].wait_recv()
        if g == 0:
            for c in loads[2:]:
                c.wait()

        def inner(f, carry):
            lanes = pl.ds(pl.multiple_of(f * ff_tile, ff_tile), ff_tile)
            x = arrived[pl.ds(g * size, size)].reshape(size * cap, depth)
            gate_act = jnp.dot(x, gate[:, lanes], preferred_element_type=f32)
            up_act = jnp.dot(x, up[:, lanes], preferred_element_type=f32)
            hidden[:, lanes] = (jax.nn.silu(gate_act) * up_act).astype(bf16)
            return carry

        lax.fori_loop(0, ff // ff_tile, inner, 0)

        def outer(q, carry):
            block = cols(lax.rem(tp + 1 + q, n_tp))
            got = jnp.dot(hidden[...], down[:, block], preferred_element_type=f32).astype(bf16)
            part[pl.ds(g * size, size), :, block] = got.reshape(size, cap, width)
            return carry

        lax.fori_loop(0, n_tp, outer, 0)

    back = {}

    def send_back(d):
        total = reduce_last(part, lead_of(d), bufs_of(d), reduced[d])
        summed[d] = total.astype(bf16)
        if d > 0:
            back[d] = go(
                remote(
                    summed.at[d],
                    returned.at[d - 1],
                    ret_send.at[d - 1],
                    ret_recv.at[d - 1],
                    (lax.rem(sp + n_sp - reach[d], n_sp), tp),
                )
            )

    def take(g):
        for d in group(g):
            if d > 0:
                back[d].wait_recv()
            block = returned[d - 1] if d > 0 else summed[0]
            expert = lax.rem(sp + reach[d], n_sp)
            want = (lax.broadcasted_iota(jnp.int32, (tok, cap), 1) + expert * cap).astype(f32)
            gives = None if d == 0 else acc[...]
            for k in range(top):
                onehot = jnp.where(want == slots[k], 1.0, 0.0).astype(bf16)
                term = jnp.dot(onehot, block, preferred_element_type=f32)
                term = term * weights[k]
                gives = term if gives is None else gives + term
            acc[...] = gives

    reduced = {}
    for step in range(GROUPS + 5):
        if step < GROUPS:
            for d in group(step):
                if d > 0:
                    gather_first(d)
        if 1 <= step < GROUPS + 1:
            for d in group(step - 1):
                gather_second(d)
        if 2 <= step < GROUPS + 2:
            experts(step - 2)
            for d in group(step - 2):
                reduced[d] = reduce_first(part, lead_of(d), bufs_of(d), d)
        if 3 <= step < GROUPS + 3:
            for d in group(step - 3):
                reduce_second(part, lead_of(d), bufs_of(d), d, reduced[d])
        if 4 <= step < GROUPS + 4:
            for d in group(step - 4):
                send_back(d)
        if 5 <= step:
            take(step - 5)

    joined[...] = (stream[...].astype(f32) + acc[...]).astype(bf16)
    last = []
    for q in range(1, n_tp):
        peer = lax.rem(tp + q, n_tp)
        there = pl.ds(pl.multiple_of(peer * rows, rows), rows)
        last.append(
            go(
                remote(
                    joined.at[there],
                    out.at[:, mine],
                    last_send.at[q - 1],
                    last_recv.at[q - 1],
                    (sp, peer),
                )
            )
        )
    out[:, mine] = joined[pl.ds(pl.multiple_of(tp * rows, rows), rows), :]
    for c in last:
        c.wait_recv()
    for c in sent:
        c.wait_send()


def vmem(count):
    return [pl.BlockSpec(memory_space=pltpu.VMEM)] * count


def per_device(
    query_rows,
    key_rows,
    value_rows,
    sink_logits,
    out_weight,
    stream_in,
    norm_gain,
    routes,
    route_weights,
    gate_weight,
    up_weight,
    down_weight,
):
    n_sp = lax.axis_size("sp")
    n_tp = lax.axis_size("tp")
    tok_count = query_rows.shape[0]
    local_heads = query_rows.shape[1] // HEAD_DIM
    depth = stream_in.shape[1]
    width = depth // n_tp
    half = width // 2
    row_share = tok_count // n_tp
    ff = gate_weight.shape[2]
    top_count = routes.shape[1]
    slot_cap = -(-3 * tok_count * top_count // (2 * n_sp) // 16) * 16
    bf16 = jnp.bfloat16
    f32 = jnp.float32
    size = n_sp // GROUPS
    blocks = tok_count // WINDOW
    dma = pltpu.SemaphoreType.DMA
    buf = pltpu.VMEM
    if n_tp == 4:
        first0, first = (blocks, 2, WINDOW, half), (n_sp, 2, slot_cap, half)
        second0, second = (blocks, WINDOW, half), (n_sp, slot_cap, half)
    else:
        first0 = (blocks, n_tp - 1, WINDOW, width)
        first = (n_sp, n_tp - 1, slot_cap, width)
        second0, second = (blocks, 16, 128), (n_sp, 16, 128)
    few = max(6, n_tp - 1)
    any_spec = pl.BlockSpec(memory_space=pl.ANY)
    return pl.pallas_call(
        functools.partial(layer_kernel, n_sp, n_tp),
        out_shape=jax.ShapeDtypeStruct((row_share, depth), bf16),
        in_specs=vmem(7) + [any_spec] * 5,
        out_specs=vmem(1)[0],
        scratch_shapes=[
            buf((2, WINDOW, 2 * HEAD_DIM), bf16),
            buf((tok_count, local_heads * HEAD_DIM), bf16),
            buf(out_weight.shape, bf16),
            buf((tok_count, width), bf16),
            buf((depth, ff), bf16),
            buf((depth, ff), bf16),
            buf((ff, depth), bf16),
            buf((tok_count, depth), bf16),
            buf(first0, bf16),
            buf(first0 if n_tp == 4 else second0, bf16),
            buf(second0, bf16),
            buf(second0, bf16),
            buf(second0, bf16),
            buf(second0, bf16),
            buf((tok_count, width), bf16),
            buf((8, tok_count), f32),
            buf((n_tp - 1, 8, tok_count), f32),
            buf((n_sp - 1, slot_cap, width), bf16),
            buf((n_sp, slot_cap, depth), bf16),
            buf((size * slot_cap, ff), bf16),
            buf((n_sp, slot_cap, depth), bf16),
            buf(first, bf16),
            buf(first if n_tp == 4 else second, bf16),
            buf(second, bf16),
            buf(second, bf16),
            buf(second, bf16),
            buf(second, bf16),
            buf((n_sp, slot_cap, width), bf16),
            buf((n_sp - 1, slot_cap, width), bf16),
            buf((tok_count, width), f32),
            buf((tok_count, width), bf16),
            dma((2, 2)),
            dma((5,)),
            dma((n_sp + blocks, few)),
            dma((n_sp + blocks, few)),
            dma((n_tp - 1,)),
            dma((n_tp - 1,)),
            dma((n_sp - 1,)),
            dma((n_sp - 1,)),
            dma((n_sp, few)),
            dma((n_sp, few)),
            dma((n_sp - 1,)),
            dma((n_sp - 1,)),
            dma((n_tp - 1,)),
            dma((n_tp - 1,)),
        ],
        compiler_params=pltpu.CompilerParams(
            collective_id=0, has_side_effects=True, vmem_limit_bytes=58 << 20
        ),
        name="layer",
    )(
        query_rows,
        key_rows,
        value_rows,
        sink_logits.reshape(1, local_heads),
        norm_gain.reshape(1, depth),
        jnp.transpose(routes),
        jnp.transpose(route_weights),
        out_weight,
        stream_in,
        gate_weight,
        up_weight,
        down_weight,
    )


def solution(mesh):
    return jax.shard_map(
        per_device,
        mesh=mesh,
        in_specs=(
            P("sp", "tp"),
            P("sp", None),
            P("sp", None),
            P("tp"),
            P("tp", None),
            P("sp", None),
            P(),
            P("sp", None),
            P("sp", None),
            P("sp", None, "tp"),
            P("sp", None, "tp"),
            P("sp", "tp", None),
        ),
        out_specs=P(("sp", "tp"), None),
        check_vma=False,
    )
```
